32 devices in a mesh: sp: 8 (over z, x), tp: 4 (over y, core).
Axes of the slice: x: 2, y: 2, z: 4, core: 2. Of those that a mesh axis runs over, the one named last changes fastest.
Arguments:
- stream: bfloat16 [8192, 2048], P(('sp', 'tp')), may hold values from -6 to 6
- mixer_input: bfloat16 [8192, 1024], P('sp', 'tp'), may hold values from -6 to 6
- document_ids: int32 [8192], P('sp'), may hold values from 0 to 3, never falling along the last dimension, each value on 1 to 4096 neighbouring positions
- decay_rate: float32 [64, 64], P('tp'), may hold values from 6.1035156e-05 to 0.015625
- rotation: float32 [64, 64], P('tp'), may hold values from -3.140625 to 3.140625
- forget_log: float32 [8192, 64], P('sp', 'tp'), may hold values from -1 to 0
- input_map: bfloat16 [2, 64, 64, 16], P(None, 'tp'), may hold values from -1.5 to 1.5
- readout_map: bfloat16 [2, 64, 16, 64], P(None, 'tp'), may hold values from -0.5 to 0.5
- skip_gain: float32 [64, 16], P('tp'), may hold values from -3 to 3
- out_projection: bfloat16 [1024, 2048], replicated, may hold values from -0.1875 to 0.1875
- norm_gain: float32 [2048], replicated, may hold values from 0.1 to 1.9
- expert_ids: int32 [8192, 8], P('sp'), may hold values from 0 to 31, all different within a row; in each aligned block of 1024 rows (0 to 1023, 1024 to 2047, ...) at most 512 rows name the same one
- route_weight: float32 [8192, 8], P('sp'), may hold values from 0.05 to 1
- expert_gate: bfloat16 [32, 2048, 512], P(('sp', 'tp')), may hold values from -0.125 to 0.125
- expert_up: bfloat16 [32, 2048, 512], P(('sp', 'tp')), may hold values from -0.125 to 0.125
- expert_down: bfloat16 [32, 512, 2048], P(('sp', 'tp')), may hold values from -0.25 to 0.25
- shared_gate: bfloat16 [2048, 512], P(None, 'tp'), may hold values from -0.125 to 0.125
- shared_up: bfloat16 [2048, 512], P(None, 'tp'), may hold values from -0.125 to 0.125
- shared_down: bfloat16 [512, 2048], P('tp'), may hold values from -0.25 to 0.25
Outputs:
- layer_out: bfloat16 [8192, 2048], P(('sp', 'tp'))
The draws below stay inside these ranges and needn't reach their ends.
Inputs may be any that keep to these rules, and one draw needn't show every extreme that they name: `expert_ids`: each row names 8 different experts. In the rows of one device (aligned blocks of 1024 rows) no expert is named by more than 512 rows. `document_ids`: never falling along the positions; each document covers 1 to 4096 positions.
All inputs are finite; a program needn't handle non-finite values.
Results may differ from the reference program's by a relative error of at most 0.018.
Values may be sent and summed in bfloat16 or wider, within the bound.
A program may use at most 256 MiB of HBM per device.

```python
import math
import jax
import jax.numpy as jnp
import numpy as np
from jax import lax

D = 2048
SSM_WIDTH = 1024
GROUP = 16
STATE = 64
EFF = 512
SFF = 512
TOP_K = 8
TOK_DEV = 1024
TOKEN_POSITIONS = 8192
SSM_GROUPS = 64
EXPERTS = 32
CAP = 512
DOCS = 4
DOC_MOST = 4096
N_SP = 8
N_TP = 4


def draw_decay_rate(key, part):
    random_key_split = jax.random.split(key, 3)
    fast_share = 0.5
    is_fast = jax.random.uniform(random_key_split[0], (SSM_GROUPS, STATE), jnp.float32) < fast_share
    fast_rate = jnp.exp(jax.random.uniform(random_key_split[1], (SSM_GROUPS, STATE), jnp.float32, math.log(4.0 / TOK_DEV), math.log(16.0 / TOK_DEV)))
    slow_rate = jnp.exp(jax.random.uniform(random_key_split[2], (SSM_GROUPS, STATE), jnp.float32, math.log(0.25 / DOC_MOST), math.log(1.0 / DOC_MOST)))
    return jnp.where(is_fast, fast_rate, slow_rate).astype(jnp.float32)


def draw_forget_log(key, part):
    random_key_split = jax.random.split(key, 4)
    blocks = TOKEN_POSITIONS // TOK_DEV
    lowest_factor = 0.2
    highest_factor = 3.0
    factor = jnp.exp(jax.random.uniform(random_key_split[0], (blocks, SSM_GROUPS), jnp.float32, math.log(lowest_factor), math.log(highest_factor)))
    factor = jnp.repeat(factor, TOK_DEV, axis=0)
    roughness = jax.random.uniform(random_key_split[1], (TOKEN_POSITIONS, SSM_GROUPS), jnp.float32, 0.5, 1.5)
    reference_level = -factor * roughness / DOC_MOST
    spike_location = jax.random.randint(random_key_split[2], (3,), 0, TOKEN_POSITIONS)
    spike_flag = jnp.any(jnp.arange(TOKEN_POSITIONS)[:, None] == spike_location[None, :], axis=1)
    spike_amplitude = jax.random.uniform(random_key_split[3], (TOKEN_POSITIONS, 1), jnp.float32, math.log(0.5), math.log(0.8))
    return jnp.where(spike_flag[:, None], reference_level + spike_amplitude, reference_level).astype(jnp.float32)


def block_levels(own_key, dims, cuts, low, largest):
    def one(dim, shards_of):
        draws = jax.random.uniform(jax.random.fold_in(jax.random.fold_in(own_key, 6), dim), (shards_of,), jnp.float32, low / len(cuts), largest / len(cuts))
        return jnp.repeat(jnp.exp(draws), dims[dim] // shards_of).reshape((-1,) + (1,) * (len(dims) - dim - 1))

    level = one(*cuts[0])
    for cut in cuts[1:]:
        level = level * one(*cut)
    return level


def length_profile(count, total, bound, slope):
    loads = [(1 << 20) // math.isqrt(standing ** slope) + 1 for standing in range(2, count + 1)]
    spare, given = total - bound - (count - 1), [1] * (count - 1)
    while spare > 0:
        free = [i for i in range(count - 1) if given[i] < bound]
        pool, budget = sum([loads[i] for i in free]), spare
        for i in free:
            more = min(bound - given[i], max(1, budget * loads[i] // pool), spare)
            given[i] = given[i] + more
            spare = spare - more
    return np.array([bound] + given)


def ragged(stream_key, amount, total, most, lean):
    if amount == 2:
        one = jax.random.randint(stream_key, (), max(1, total - most), min(most, total - 1) + 1)
        return jnp.stack([one, total - one])
    sizes = jnp.asarray(length_profile(amount, total, most, lean), jnp.int32)
    couples = (amount - 1) // 2
    giver, taker = sizes[1:1 + 2 * couples:2], sizes[2:2 + 2 * couples:2]
    slack = jnp.minimum(giver - 1, most - taker)
    shifted = jax.random.randint(jax.random.fold_in(stream_key, 1), (couples,), 0, 1 << 20) % (slack + 1)
    sizes = sizes.at[1:1 + 2 * couples:2].set(giver - shifted).at[2:2 + 2 * couples:2].set(taker + shifted)
    return sizes[jax.random.permutation(jax.random.fold_in(stream_key, 2), amount)]


def deal_out(stream_key, own, number, rows, count, top, reach, skew):
    sequence = jax.random.permutation(stream_key, count)
    crowded, common = portions_of(count, rows * top, reach, skew, True), portions_of(count, rows * top, reach, skew, False)
    places = jnp.arange(count)

    def named(tallies, turn):
        used = int((tallies > 0).sum())
        fixed = max(1, used // 4)
        moved = fixed + (places - fixed + turn * (used - fixed)) % max(1, count - fixed)
        return jnp.zeros((count,), jnp.int32).at[sequence[jnp.where(places < fixed, places, moved)]].set(jnp.asarray(tallies, jnp.int32))

    tallies = jnp.where(number % 4 == 0, named(crowded, number // 4), named(common, number - number // 4 - 1))
    mixed = jax.random.permutation(jax.random.fold_in(own, 3), count)
    giver, receiver = mixed[0:count // 2 * 2:2], mixed[1:count // 2 * 2:2]
    margin = jnp.minimum(tallies[giver] - 1, reach - tallies[receiver]) // 2
    margin = jnp.where((giver == sequence[0]) | (receiver == sequence[0]) | (tallies[receiver] == 0), 0, jnp.maximum(margin, 0))
    moved = jax.random.randint(jax.random.fold_in(own, 4), (count // 2,), 0, 1 << 20) % (margin + 1)
    tallies = tallies.at[giver].add(-moved).at[receiver].add(moved)
    items = jnp.searchsorted(jnp.cumsum(tallies), jnp.arange(rows * top), side="right").astype(jnp.int32)
    grid = items.reshape(top, rows).T
    grid = grid[jax.random.permutation(jax.random.fold_in(own, 1), rows)]
    turn = jax.random.randint(jax.random.fold_in(own, 2), (rows, 1), 0, top)
    return jnp.take_along_axis(grid, (jnp.arange(top)[None, :] + turn) % top, axis=1)


def portions_of(count, total, most, skew, full):
    portions = [(1 << 20) // math.isqrt(rank ** skew) + 1 for rank in range(1, count + 1)]
    largest = most if full else min(most, max(-(-total // count), total * portions[0] // sum(portions)))
    least = 1 if total - largest >= count - 1 else 0
    given, surplus = [largest] + [least] * (count - 1), total - largest - least * (count - 1)
    while surplus > 0:
        free = [i for i in range(1, count) if given[i] < largest] or [i for i in range(1, count) if given[i] < most]
        whole, remaining = sum([portions[i] for i in free]), surplus
        for i in free:
            more = min(most - given[i], max(1, remaining * portions[i] // whole), surplus)
            given[i] = given[i] + more
            surplus = surplus - more
    return np.array(given)


def bell_draw(own_key, extent, spread, bound, cuts=(), kind=jnp.bfloat16):
    values = spread * jax.random.normal(own_key, extent, jnp.float32)
    if cuts:
        values = values * block_levels(own_key, extent, cuts, -0.22, 0.18)
    return jnp.clip(values, -bound, bound).astype(kind)


def setup_inputs(seed: int = 0) -> dict:
    arg_keys = jax.random.split(jax.random.key(seed), 20)
    stream = bell_draw(arg_keys[0], (TOKEN_POSITIONS, D), 1.0, 6.0, ((0, 32),))
    mixer_input = bell_draw(arg_keys[1], (TOKEN_POSITIONS, SSM_WIDTH), 1.0, 6.0, ((0, 8), (1, 4)))
    document_ids = jnp.searchsorted(jnp.cumsum(ragged(arg_keys[2], DOCS, TOKEN_POSITIONS, DOC_MOST, 2)), jnp.arange(TOKEN_POSITIONS), side="right").astype(jnp.int32)
    decay_rate = draw_decay_rate(jax.random.fold_in(arg_keys[19], 71), 0)
    rotation = jnp.clip(jax.random.uniform(arg_keys[4], (SSM_GROUPS, STATE), jnp.float32, -3.140625, 3.140625), -3.140625, 3.140625)
    forget_log = draw_forget_log(jax.random.fold_in(arg_keys[19], 71), 0)
    input_map = bell_draw(arg_keys[6], (2, SSM_GROUPS, STATE, GROUP), GROUP ** -0.5, 1.5, ((1, 4),))
    readout_map = bell_draw(arg_keys[7], (2, SSM_GROUPS, GROUP, STATE), (2 * STATE) ** -0.5, 0.5, ((1, 4),))
    skip_gain = bell_draw(arg_keys[8], (SSM_GROUPS, GROUP), 0.5, 3.0, ((0, 4),), jnp.float32)
    out_projection = bell_draw(arg_keys[9], (SSM_WIDTH, D), SSM_WIDTH ** -0.5, 0.1875)
    norm_gain = jnp.clip(1.0 + 0.18 * jax.random.normal(arg_keys[10], (D,), jnp.float32), 0.1, 1.9)
    expert_ids_keys = jax.random.split(jax.random.fold_in(arg_keys[11], 1), TOKEN_POSITIONS // TOK_DEV)
    expert_ids_turns = jax.random.permutation(jax.random.fold_in(arg_keys[11], 3), TOKEN_POSITIONS // TOK_DEV)
    expert_ids = jax.vmap(lambda own, number: deal_out(jax.random.fold_in(arg_keys[11], 2), own, number, TOK_DEV, EXPERTS, TOP_K, CAP, 2))(expert_ids_keys, expert_ids_turns).reshape((TOKEN_POSITIONS, TOP_K))
    route_weight = jnp.clip(jnp.exp(math.log(1.0) - 2.9957323 * jax.random.uniform(arg_keys[12], (TOKEN_POSITIONS, TOP_K), jnp.float32) ** block_levels(arg_keys[12], (TOKEN_POSITIONS, TOP_K), ((0, 8),), -0.2, 0.2)), 0.05, 1.0)
    expert_gate = bell_draw(arg_keys[13], (EXPERTS, D, EFF), D ** -0.5, 0.125, ((0, 32),))
    expert_up = bell_draw(arg_keys[14], (EXPERTS, D, EFF), D ** -0.5, 0.125, ((0, 32),))
    expert_down = bell_draw(arg_keys[15], (EXPERTS, EFF, D), EFF ** -0.5, 0.25, ((0, 32),))
    shared_gate = bell_draw(arg_keys[16], (D, SFF), D ** -0.5, 0.125, ((1, 4),))
    shared_up = bell_draw(arg_keys[17], (D, SFF), D ** -0.5, 0.125, ((1, 4),))
    shared_down = bell_draw(arg_keys[18], (SFF, D), SFF ** -0.5, 0.25, ((0, 4),))
    return dict(stream=stream, mixer_input=mixer_input, document_ids=document_ids, decay_rate=decay_rate, rotation=rotation, forget_log=forget_log, input_map=input_map, readout_map=readout_map, skip_gain=skip_gain, out_projection=out_projection, norm_gain=norm_gain, expert_ids=expert_ids, route_weight=route_weight, expert_gate=expert_gate, expert_up=expert_up, expert_down=expert_down, shared_gate=shared_gate, shared_up=shared_up, shared_down=shared_down)


norm_eps = 1e-06
highest = lax.Precision.HIGHEST

def pair_combine(earlier, later):
    a_re1, a_im1, b_re1, b_im1 = earlier
    a_re2, a_im2, b_re2, b_im2 = later
    return (a_re1 * a_re2 - a_im1 * a_im2, a_re1 * a_im2 + a_im1 * a_re2, a_re2 * b_re1 - a_im2 * b_im1 + b_re2, a_re2 * b_im1 + a_im2 * b_re1 + b_im2)

def reference(stream, mixer_input, document_ids, decay_rate, rotation, forget_log, input_map, readout_map, skip_gain, out_projection, norm_gain, expert_ids, route_weight, expert_gate, expert_up, expert_down, shared_gate, shared_up, shared_down):
    starts = jnp.concatenate([jnp.zeros((1,), bool), document_ids[1:] != document_ids[:-1]])
    input_f = mixer_input.astype(jnp.float32)
    grouped = input_f.reshape(TOKEN_POSITIONS, SSM_GROUPS, GROUP).transpose(1, 0, 2)
    in_maps = input_map.astype(jnp.float32).transpose(1, 0, 2, 3)
    out_maps = readout_map.astype(jnp.float32).transpose(1, 0, 2, 3)

    def group_scan(pieces):
        input_g, forget_g, rate_g, turn_g, in_g, out_g, skip_g = pieces
        magnitude = jnp.exp(forget_g[:, None] - rate_g[None, :])
        decay_re = jnp.where(starts[:, None], 0.0, magnitude * jnp.cos(turn_g)[None, :])
        decay_im = jnp.where(starts[:, None], 0.0, magnitude * jnp.sin(turn_g)[None, :])
        in_scale = jnp.sqrt(1.0 - jnp.exp(-2.0 * rate_g))
        driven_re = jnp.dot(input_g, in_g[0].T, precision=highest) * in_scale[None, :]
        driven_im = jnp.dot(input_g, in_g[1].T, precision=highest) * in_scale[None, :]
        scanned = lax.associative_scan(pair_combine, (decay_re, decay_im, driven_re, driven_im), axis=0)
        readout = jnp.dot(scanned[2], out_g[0].T, precision=highest) - jnp.dot(scanned[3], out_g[1].T, precision=highest) + skip_g[None, :] * input_g
        return jax.nn.gelu(readout)
    mixer_rows = lax.map(group_scan, (grouped, forget_log.T, decay_rate, rotation, in_maps, out_maps, skip_gain))
    mixer_out = mixer_rows.transpose(1, 0, 2).reshape(TOKEN_POSITIONS, SSM_WIDTH).astype(jnp.bfloat16)
    mixed = jnp.dot(mixer_out.astype(jnp.float32), out_projection.astype(jnp.float32))
    residual = (stream.astype(jnp.float32) + mixed).astype(jnp.bfloat16)
    resid_f = residual.astype(jnp.float32)
    normed = (resid_f * lax.rsqrt(lax.optimization_barrier(jnp.mean(resid_f * resid_f, axis=-1, keepdims=True)) + norm_eps) * norm_gain[None, :]).astype(jnp.bfloat16)
    normed_f = normed.astype(jnp.float32)
    normed_pad = jnp.concatenate([normed_f, jnp.zeros((1, D), jnp.float32)])
    flat_expert = expert_ids.reshape(-1).astype(jnp.int32)
    flat_weight = route_weight.reshape(-1)
    sorted_slots = jnp.argsort(flat_expert, stable=True).astype(jnp.int32)
    counts = jnp.bincount(flat_expert, length=EXPERTS).astype(jnp.int32)
    offsets = (jnp.cumsum(counts) - counts).astype(jnp.int32)
    slot_range = jnp.arange(N_SP * CAP, dtype=jnp.int32)

    def expert_pass(expert, routed_sum):
        is_live = slot_range < counts[expert]
        position = sorted_slots[jnp.minimum(offsets[expert] + slot_range, TOKEN_POSITIONS * TOP_K - 1)]
        token_table = jnp.where(is_live, position // TOP_K, TOKEN_POSITIONS).astype(jnp.int32)
        weight_table = jnp.where(is_live, flat_weight[position], 0.0)
        row_block = normed_pad[token_table]
        gate_value = jnp.dot(row_block, expert_gate[expert].astype(jnp.float32))
        up_value = jnp.dot(row_block, expert_up[expert].astype(jnp.float32))
        hidden = lax.optimization_barrier((jax.nn.silu(gate_value) * up_value).astype(jnp.bfloat16))
        expert_rows = jnp.dot(hidden.astype(jnp.float32), expert_down[expert].astype(jnp.float32)).astype(jnp.bfloat16)
        return routed_sum.at[token_table].add(weight_table[:, None] * expert_rows.astype(jnp.float32), mode='drop')
    block_width = SFF // N_TP
    total = resid_f
    for column in range(N_TP):
        routed_sum = lax.fori_loop(0, N_SP, lambda source, acc_sum: expert_pass(source * N_TP + column, acc_sum), jnp.zeros((TOKEN_POSITIONS, D), jnp.float32))
        lower = column * block_width
        gate_block = jnp.dot(normed_f, shared_gate[:, lower:lower + block_width].astype(jnp.float32))
        up_block = jnp.dot(normed_f, shared_up[:, lower:lower + block_width].astype(jnp.float32))
        shared_hidden = lax.optimization_barrier((jax.nn.silu(gate_block) * up_block).astype(jnp.bfloat16))
        shared_part = jnp.dot(shared_hidden.astype(jnp.float32), shared_down[lower:lower + block_width].astype(jnp.float32))
        partial_value = lax.optimization_barrier((routed_sum + shared_part).astype(jnp.bfloat16))
        total = total + partial_value.astype(jnp.float32)
    return total.astype(jnp.bfloat16)
```

```python
import functools
import math

import jax
import jax.numpy as jnp
from jax import lax
from jax.experimental import pallas as pl
from jax.experimental.pallas import tpu as pltpu
from jax.sharding import PartitionSpec as P

norm_eps = 1e-06
highest = lax.Precision.HIGHEST
lanes_at_once = 512
chunks = 8
longest_ring = 16


def decayed(e, lam_re, lam_im, d_re, d_im, h_re, h_im):
    a_re, a_im = e * lam_re, e * lam_im
    return a_re * h_re - a_im * h_im + d_re, a_re * h_im + a_im * h_re + d_im


def column_blocks(width):
    size = min(lanes_at_once, width)
    return [(c, size) for c in range(0, width, size)]


def wide(row, size):
    return jnp.broadcast_to(row, (chunks, size))


def ends_kernel(e_ref, d_ref, lam_ref, docs_ref, chunk_ref, summary_ref):
    positions, width = e_ref.shape
    length = positions // chunks
    for c, size in column_blocks(width):
        lam_re = wide(lam_ref[0:1, c : c + size], size)
        lam_im = wide(lam_ref[1:2, c : c + size], size)

        def step(i, carry):
            h_re, h_im, gain = carry
            for k in range(4):
                r = pl.ds(pl.multiple_of((i * 4 + k) * chunks, chunks), chunks)
                e = e_ref[r, c : c + size]
                h_re, h_im = decayed(
                    e,
                    lam_re,
                    lam_im,
                    d_ref[r, c : c + size],
                    d_ref[r, width + c : width + c + size],
                    h_re,
                    h_im,
                )
                gain = gain * e
            return h_re, h_im, gain

        zero = jnp.zeros((chunks, size), jnp.float32)
        h_re, h_im, gain = lax.fori_loop(0, length // 4, step, (zero, zero, zero + 1.0))
        p_re = gain * lam_ref[2:3, c : c + size]
        p_im = gain * lam_ref[3:4, c : c + size]
        for k, part in enumerate((p_re, p_im, h_re, h_im)):
            chunk_ref[k * chunks : (k + 1) * chunks, c : c + size] = part
        q_re, q_im = p_re[0:1], p_im[0:1]
        s_re, s_im = h_re[0:1], h_im[0:1]
        for j in range(1, chunks):
            a_re, a_im = p_re[j : j + 1], p_im[j : j + 1]
            q_re, q_im = a_re * q_re - a_im * q_im, a_re * q_im + a_im * q_re
            s_re, s_im = (
                a_re * s_re - a_im * s_im + h_re[j : j + 1],
                a_re * s_im + a_im * s_re + h_im[j : j + 1],
            )
        summary_ref[:, c : c + size] = jnp.concatenate(
            [q_re, q_im, s_re, s_im, docs_ref[0:4, c : c + size]], axis=0
        )


def states_kernel(me_ref, e_ref, d_ref, lam_ref, chunk_ref, all_ref, out_ref):
    positions, width = e_ref.shape
    length = positions // chunks
    peers = all_ref.shape[0]
    me = me_ref[0]
    for c, size in column_blocks(width):
        lam_re = wide(lam_ref[0:1, c : c + size], size)
        lam_im = wide(lam_ref[1:2, c : c + size], size)
        s_re = jnp.zeros((1, size), jnp.float32)
        s_im = jnp.zeros((1, size), jnp.float32)
        last = jnp.full((1, size), -1.0, jnp.float32)
        for k in range(peers - 1, 0, -1):
            row = all_ref[k, :, c : c + size]
            a_re, a_im = row[0:1], row[1:2]
            keep = jnp.where(row[4:5] == last, 1.0, 0.0)
            n_re = keep * (a_re * s_re - a_im * s_im) + row[2:3]
            n_im = keep * (a_re * s_im + a_im * s_re) + row[3:4]
            s_re = jnp.where(me >= k, n_re, s_re)
            s_im = jnp.where(me >= k, n_im, s_im)
            last = jnp.where(me >= k, row[5:6], last)
        keep = jnp.where(all_ref[0, 4:5, c : c + size] == last, 1.0, 0.0)
        s_re, s_im = keep * s_re, keep * s_im
        starts_re, starts_im = [s_re], [s_im]
        parts = [chunk_ref[k * chunks : (k + 1) * chunks, c : c + size] for k in range(4)]
        for j in range(chunks - 1):
            a_re, a_im, b_re, b_im = (part[j : j + 1] for part in parts)
            s_re, s_im = a_re * s_re - a_im * s_im + b_re, a_re * s_im + a_im * s_re + b_im
            starts_re.append(s_re)
            starts_im.append(s_im)

        def step(i, carry):
            h_re, h_im = carry
            for pair in range(2):
                kept_re, kept_im = [], []
                for k in range(2):
                    r = pl.ds(pl.multiple_of((i * 4 + pair * 2 + k) * chunks, chunks), chunks)
                    h_re, h_im = decayed(
                        e_ref[r, c : c + size],
                        lam_re,
                        lam_im,
                        d_ref[r, c : c + size],
                        d_ref[r, width + c : width + c + size],
                        h_re,
                        h_im,
                    )
                    kept_re.append(h_re)
                    kept_im.append(h_im)
                both = pl.ds(pl.multiple_of((i * 2 + pair) * 2 * chunks, 2 * chunks), 2 * chunks)
                out_ref[both, c : c + size] = jnp.concatenate(kept_re, axis=0).astype(jnp.bfloat16)
                out_ref[both, width + c : width + c + size] = jnp.concatenate(
                    kept_im, axis=0
                ).astype(jnp.bfloat16)
            return h_re, h_im

        lax.fori_loop(
            0,
            length // 4,
            step,
            (jnp.concatenate(starts_re, axis=0), jnp.concatenate(starts_im, axis=0)),
        )


vmem = pl.BlockSpec(memory_space=pltpu.VMEM)
smem = pl.BlockSpec(memory_space=pltpu.SMEM)
params = pltpu.CompilerParams(vmem_limit_bytes=40 * 1024 * 1024)


def ring_order(count):
    across = 1 << (int(math.log2(count)) // 2)
    along = count // across
    walk = [(z, 0) for z in range(along)]
    for x in range(1, across):
        column = range(1, along) if x % 2 == 0 else range(along - 1, 0, -1)
        walk += [(z, x) for z in column]
    walk += [(0, x) for x in range(across - 1, 0, -1)]
    return [z * across + x for z, x in walk]


def interleave(rows):
    positions = rows.shape[0]
    return (
        rows.reshape((chunks, positions // chunks) + rows.shape[1:])
        .swapaxes(0, 1)
        .reshape(rows.shape)
    )


def deinterleave(rows):
    positions = rows.shape[0]
    return (
        rows.reshape((positions // chunks, chunks) + rows.shape[1:])
        .swapaxes(0, 1)
        .reshape(rows.shape)
    )


def mixer(mixer_input, document_ids, decay_rate, rotation, forget_log, input_map, readout_map, skip_gain):
    positions = mixer_input.shape[0]
    groups_here, states = decay_rate.shape
    group_size = skip_gain.shape[1]
    width = groups_here * states
    channels = groups_here * group_size
    length = positions // chunks
    peers, mine = lax.axis_size("sp"), lax.axis_index("sp")
    starts = jnp.concatenate([jnp.zeros((1,), bool), document_ids[1:] != document_ids[:-1]])
    gain = interleave(jnp.where(starts[:, None], 0.0, jnp.exp(forget_log)))
    column_group = jnp.arange(width, dtype=jnp.int32) // states
    spread = (jnp.arange(groups_here, dtype=jnp.int32)[:, None] == column_group[None, :]).astype(
        jnp.float32
    )
    gain_wide = jnp.dot(gain, spread, precision=highest, preferred_element_type=jnp.float32)
    rows = interleave(mixer_input)
    row_group = jnp.arange(channels, dtype=jnp.int32) // group_size
    same_group = row_group[:, None, None] == column_group.reshape(1, groups_here, states)[:, :, :1]
    maps = input_map.transpose(1, 3, 0, 2).reshape(channels, 2, 1, states)
    in_wide = jnp.where(same_group[:, None], maps, jnp.zeros((), maps.dtype)).reshape(
        channels, 2 * width
    )
    in_scale = jnp.sqrt(1.0 - jnp.exp(-2.0 * decay_rate)).reshape(1, width)
    driven = jnp.dot(rows, in_wide, preferred_element_type=jnp.float32) * jnp.concatenate(
        [in_scale, in_scale], axis=1
    )
    rate, turn = decay_rate.reshape(1, width), rotation.reshape(1, width)
    one_re, one_im = jnp.exp(-rate) * jnp.cos(turn), jnp.exp(-rate) * jnp.sin(turn)
    all_re, all_im, square = one_re, one_im, length
    while square > 1:
        all_re, all_im = all_re * all_re - all_im * all_im, 2.0 * all_re * all_im
        square //= 2
    lam = jnp.concatenate([one_re, one_im, all_re, all_im], axis=0)
    docs = jnp.stack([document_ids[0], document_ids[-1], document_ids[0], document_ids[-1]])
    docs = jnp.broadcast_to(docs.astype(jnp.float32)[:, None], (4, width))
    chunk_ends, summary = pl.pallas_call(
        ends_kernel,
        out_shape=(
            jax.ShapeDtypeStruct((4 * chunks, width), jnp.float32),
            jax.ShapeDtypeStruct((8, width), jnp.float32),
        ),
        in_specs=[vmem] * 4,
        out_specs=(vmem, vmem),
        compiler_params=params,
        cost_estimate=pl.CostEstimate(
            flops=12 * positions * width, bytes_accessed=12 * positions * width, transcendentals=0
        ),
    )(gain_wide, driven, lam, docs)
    earlier = [summary] + [
        lax.ppermute(summary, "sp", [(i, (i + k) % peers) for i in range(peers)])
        for k in range(1, peers)
    ]
    held = pl.pallas_call(
        states_kernel,
        out_shape=jax.ShapeDtypeStruct((positions, 2 * width), jnp.bfloat16),
        in_specs=[smem] + [vmem] * 5,
        out_specs=vmem,
        compiler_params=params,
        cost_estimate=pl.CostEstimate(
            flops=12 * positions * width, bytes_accessed=16 * positions * width, transcendentals=0
        ),
    )(mine[None].astype(jnp.int32), gain_wide, driven, lam, chunk_ends, jnp.stack(earlier))
    signs = jnp.stack([readout_map[0], -readout_map[1]])
    outs = signs.transpose(0, 1, 3, 2).reshape(2, groups_here, states, 1, group_size)
    own = jnp.arange(groups_here)[:, None] == jnp.arange(groups_here)[None, :]
    out_wide = jnp.where(own[None, :, None, :, None], outs, jnp.zeros((), outs.dtype)).reshape(
        2 * width, channels
    )
    readout = jnp.dot(held, out_wide, preferred_element_type=jnp.float32)
    readout = readout + skip_gain.reshape(1, channels) * rows.astype(jnp.float32)
    return deinterleave(jax.nn.gelu(readout).astype(jnp.bfloat16))


def spread_over_tp(block):
    members = lax.axis_size("tp")
    blocks, offsets, bit = [block], [0], members // 2
    while bit:
        pairs = [(i, i ^ bit) for i in range(members)]
        blocks = blocks + [lax.ppermute(item, "tp", pairs) for item in blocks]
        offsets = offsets + [offset ^ bit for offset in offsets]
        bit //= 2
    return blocks, offsets


def body(
    stream,
    mixer_input,
    document_ids,
    decay_rate,
    rotation,
    forget_log,
    input_map,
    readout_map,
    skip_gain,
    out_projection,
    norm_gain,
    expert_ids,
    route_weight,
    expert_gate,
    expert_up,
    expert_down,
    shared_gate,
    shared_up,
    shared_down,
):
    sp_count, tp_count = lax.axis_size("sp"), lax.axis_size("tp")
    row, column = lax.axis_index("sp"), lax.axis_index("tp")
    own_rows = stream.shape[0]
    experts = sp_count * tp_count * expert_gate.shape[0]

    gates, offsets = spread_over_tp(expert_gate[0])
    ups, _ = spread_over_tp(expert_up[0])
    downs, _ = spread_over_tp(expert_down[0])
    gate_all = jnp.concatenate(gates, axis=1)
    up_all = jnp.concatenate(ups, axis=1)
    down_all = jnp.concatenate(downs, axis=0)
    hidden_units = gates[0].shape[1]

    ids = lax.dynamic_slice_in_dim(expert_ids, column * own_rows, own_rows, axis=0)
    weights = lax.dynamic_slice_in_dim(route_weight, column * own_rows, own_rows, axis=0)
    lanes = max(128, experts)
    named = ids[:, :, None] == jnp.arange(lanes, dtype=jnp.int32)[None, None, :]
    own_table = jnp.sum(jnp.where(named, weights[:, :, None], 0.0), axis=1)
    table = lax.all_gather(own_table, "sp", axis=0, tiled=False)
    here = row * tp_count + jnp.stack([column ^ offset for offset in offsets])
    table = jnp.take(table, here, axis=2)

    mixer_out = mixer(
        mixer_input, document_ids, decay_rate, rotation, forget_log, input_map, readout_map, skip_gain
    )
    whole_rows = lax.all_to_all(mixer_out, "tp", split_axis=0, concat_axis=1, tiled=True)
    mixed = jnp.dot(whole_rows, out_projection, preferred_element_type=jnp.float32)
    residual = (stream.astype(jnp.float32) + mixed).astype(jnp.bfloat16)
    resid_f = residual.astype(jnp.float32)
    normed = (
        resid_f
        * lax.rsqrt(jnp.mean(resid_f * resid_f, axis=-1, keepdims=True) + norm_eps)
        * norm_gain[None, :]
    ).astype(jnp.bfloat16)

    order = ring_order(sp_count)
    place = [0] * sp_count
    for k, index in enumerate(order):
        place[index] = k
    forward = [(order[k], order[(k + 1) % sp_count]) for k in range(sp_count)]
    backward = [(b, a) for a, b in forward]
    my_place = jnp.array(place, jnp.int32)[row]
    owner = jnp.array(order, jnp.int32)
    half = own_rows // 2

    def weights_of(before, after):
        first = lax.dynamic_index_in_dim(table, owner[(my_place - before) % sp_count], 0, False)
        second = lax.dynamic_index_in_dim(table, owner[(my_place + after) % sp_count], 0, False)
        return jnp.concatenate([first[:half], second[half:]], axis=0)

    def contribution(rows, weight):
        gate_value = jnp.dot(rows, gate_all, preferred_element_type=jnp.float32)
        up_value = jnp.dot(rows, up_all, preferred_element_type=jnp.float32)
        scale = jnp.concatenate(
            [
                jnp.broadcast_to(weight[:, e : e + 1], (rows.shape[0], hidden_units))
                for e in range(tp_count)
            ],
            axis=1,
        )
        hidden = (jax.nn.silu(gate_value) * up_value * scale).astype(jnp.bfloat16)
        return jnp.dot(hidden, down_all, preferred_element_type=jnp.float32)

    if sp_count > longest_ring:
        every = lax.all_gather(normed, "sp", axis=0, tiled=False)
        values = lax.map(lambda pair: contribution(*pair).astype(jnp.bfloat16), (every, table))
        arrived = lax.psum_scatter(values, "sp", scatter_dimension=0, tiled=False)
        own_value = jnp.zeros(normed.shape, jnp.float32)
    else:
        up_going, down_going = normed[:half], normed[half:]
        sum_up = sum_down = None
        for k in range(1, sp_count):
            up_going = lax.ppermute(up_going, "sp", forward)
            down_going = lax.ppermute(down_going, "sp", backward)
            value = contribution(jnp.concatenate([up_going, down_going], axis=0), weights_of(k, k))
            value_up, value_down = value[:half], value[half:]
            if k > 1:
                value_up = value_up + sum_up.astype(jnp.float32)
                value_down = value_down + sum_down.astype(jnp.float32)
            sum_up = lax.ppermute(value_up.astype(jnp.bfloat16), "sp", forward)
            sum_down = lax.ppermute(value_down.astype(jnp.bfloat16), "sp", backward)
        own_value = contribution(normed, weights_of(0, 0))
        arrived = jnp.concatenate([sum_up, sum_down], axis=0)

    shards = lax.optimization_barrier((normed, shared_gate, shared_up, shared_down))[1:]
    shared_gates, _ = spread_over_tp(shards[0])
    shared_ups, _ = spread_over_tp(shards[1])
    shared_downs, _ = spread_over_tp(shards[2])
    gate_block = jnp.dot(
        normed, jnp.concatenate(shared_gates, axis=1), preferred_element_type=jnp.float32
    )
    up_block = jnp.dot(
        normed, jnp.concatenate(shared_ups, axis=1), preferred_element_type=jnp.float32
    )
    shared_hidden = (jax.nn.silu(gate_block) * up_block).astype(jnp.bfloat16)
    own_value = own_value + jnp.dot(
        shared_hidden, jnp.concatenate(shared_downs, axis=0), preferred_element_type=jnp.float32
    )
    return (resid_f + own_value + arrived.astype(jnp.float32)).astype(jnp.bfloat16)


def solution(mesh):
    placed = (
        P(("sp", "tp"), None),
        P("sp", "tp"),
        P("sp"),
        P("tp", None),
        P("tp", None),
        P("sp", "tp"),
        P(None, "tp", None, None),
        P(None, "tp", None, None),
        P("tp", None),
        P(),
        P(),
        P("sp", None),
        P("sp", None),
        P(("sp", "tp"), None, None),
        P(("sp", "tp"), None, None),
        P(("sp", "tp"), None, None),
        P(None, "tp"),
        P(None, "tp"),
        P("tp", None),
    )
    return jax.shard_map(
        body, mesh=mesh, in_specs=placed, out_specs=P(("sp", "tp"), None), check_vma=False
    )
```
